32 devices in a mesh: sp: 8 (over z, x), tp: 4 (over y, core).
Axes of the slice: x: 2, y: 2, z: 4, core: 2. Of those that a mesh axis runs over, the one named last changes fastest.
Arguments:
- query_a: bfloat16 [1024, 2048], P('sp', 'tp'), may hold values from -6 to 6
- key_a: bfloat16 [1024, 2048], P('sp', 'tp'), may hold values from -6 to 6
- value_a: bfloat16 [1024, 4096], P('sp', 'tp'), may hold values from -6 to 6
- query_b: bfloat16 [1024, 2048], P('sp', 'tp'), may hold values from -6 to 6
- key_b: bfloat16 [1024, 2048], P('sp', 'tp'), may hold values from -6 to 6
- value_b: bfloat16 [1024, 2048], P('sp', 'tp'), may hold values from -6 to 6
- in_gate: float32 [2, 2, 16, 1024], P(None, None, 'tp', 'sp'), may hold values from -6 to 300
- forget_gate: float32 [2, 2, 16, 1024], P(None, None, 'tp', 'sp'), may hold values from 0 to 14.1
- head_gain_a: float32 [16, 256], P('tp'), may hold values from 0.1 to 1.9
- head_gain_b: float32 [16, 128], P('tp'), may hold values from 0.1 to 1.9
- out_weight_a: bfloat16 [4096, 2048], P('tp'), may hold values from -0.078125 to 0.078125
- out_weight_b: bfloat16 [2048, 2048], P('tp'), may hold values from -0.078125 to 0.078125
- residual: bfloat16 [2048, 1024], P('tp', 'sp'), may hold values from -40 to 40
- norm_gain: float32 [2048], P('tp'), may hold values from 0.1 to 1.9
- routes: int32 [1024, 2], P('sp'), may hold values from 0 to 7, all different within a row; in each aligned block of 128 rows (0 to 127, 128 to 255, ...) at most 64 rows name the same one
- route_weights: float32 [1024, 2], P('sp'), may hold values from 0.2 to 1
- expert_gate: bfloat16 [8, 2048, 4096], P('sp', None, 'tp'), may hold values from -0.125 to 0.125
- expert_up: bfloat16 [8, 2048, 4096], P('sp', None, 'tp'), may hold values from -0.125 to 0.125
- expert_down: bfloat16 [8, 4096, 2048], P('sp', 'tp'), may hold values from -0.09375 to 0.09375
Outputs:
- layer_output: bfloat16 [2048, 1024], P('tp', 'sp')
The draws below stay inside these ranges and needn't reach their ends.
Inputs may be any that keep to these rules, and one draw needn't show every extreme that they name: `routes`: each row names 2 different experts. In each aligned block of 128 rows (the rows of one index of sp) no expert is named by more than 64 rows, a bound that some blocks reach.
All inputs are finite; a program needn't handle non-finite values.
Results may differ from the reference program's by a relative error of at most 0.012.
Values may be sent and summed in bfloat16 or wider, within the bound.
A program may use at most 128 MiB of HBM per device.

```python
import math
import jax
import jax.numpy as jnp
import numpy as np
from jax import lax

D = 2048
HEAD_TOTAL = 16
DK = 128
DVA = 256
DVB = 128
BLOCK = 128
FF = 4096
TOP = 2
TOK_DEV = 128
TOKEN_TOTAL = 1024
EXPERTS = 8
SLOTS = 64
N_SP = 8
N_TP = 4


def draw_in_gate(key, part):
    base_key = jax.random.fold_in(key, 101)
    shape = (2, 2, HEAD_TOTAL, TOKEN_TOTAL)
    values = jax.random.uniform(base_key, shape, jnp.float32, -6.0, 0.0)
    return values


def draw_forget_gate(key, part):
    kind_key = jax.random.fold_in(key, 201)
    noise_key = jax.random.fold_in(key, 202)
    span_key = jax.random.fold_in(key, 203)
    spike_random_key = jax.random.fold_in(key, 204)
    depth_key = jax.random.fold_in(key, 205)
    shape = (2, 2, HEAD_TOTAL, TOKEN_TOTAL)
    spans = TOKEN_TOTAL // TOK_DEV
    quick = jax.random.randint(kind_key, (2, 2, HEAD_TOTAL, 1), 0, 2) == 1
    base = jnp.where(quick, 3.5, 11.0)
    offset = jax.random.uniform(span_key, (2, 2, HEAD_TOTAL, spans, 1), jnp.float32, -0.7, 0.7)
    offset = jnp.broadcast_to(offset, (2, 2, HEAD_TOTAL, spans, TOK_DEV)).reshape(shape)
    noise = jnp.clip(0.8 * jax.random.normal(noise_key, shape, jnp.float32), -2.4, 2.4)
    values = base + offset + noise
    spike_location = jax.random.randint(spike_random_key, (2, 2, HEAD_TOTAL, 3), 0, TOKEN_TOTAL)
    token_positions = jnp.arange(TOKEN_TOTAL, dtype=jnp.int32)
    spiked_rows = jnp.any(token_positions[None, None, None, :, None] == spike_location[:, :, :, None, :], axis=-1)
    depth = jax.random.uniform(depth_key, shape, jnp.float32, 0.0, 1.4)
    return jnp.where(spiked_rows & jnp.logical_not(quick), depth, values)


def draw_residual(key, part):
    noise_key = jax.random.fold_in(key, 301)
    scale_key = jax.random.fold_in(key, 302)
    fractions = jnp.arange(D, dtype=jnp.float32) / D
    token_scale = jnp.exp(jax.random.uniform(scale_key, (1, TOKEN_TOTAL), jnp.float32, math.log(0.3), math.log(3.0)))
    feature_scale = jnp.power(10.0, fractions - 0.5)
    values = jnp.clip(jax.random.normal(noise_key, (D, TOKEN_TOTAL), jnp.float32), -4.0, 4.0)
    return (values * feature_scale[:, None] * token_scale).astype(jnp.bfloat16)


def shard_levels(rng, extent, cuts, least, largest):
    gain = 1.0
    for axis_at, blocks in cuts:
        heights = jax.random.uniform(jax.random.fold_in(jax.random.fold_in(rng, 6), axis_at), (blocks,), jnp.float32, least / len(cuts), largest / len(cuts))
        gain = gain * jnp.repeat(jnp.exp(heights), extent[axis_at] // blocks).reshape((-1,) + (1,) * (len(extent) - 1 - axis_at))
    return gain


def deal_out(key, own, number, rows, count, top, reach, skew):
    sequence = jax.random.permutation(key, count)
    packed, common = shares(count, rows * top, reach, skew, True), shares(count, rows * top, reach, skew, False)
    places = jnp.arange(count)

    def named(tallies, rotation):
        used = int((tallies > 0).sum())
        fixed = max(1, used // 4)
        passed = fixed + (places - fixed + rotation * (used - fixed)) % max(1, count - fixed)
        return jnp.zeros((count,), jnp.int32).at[sequence[jnp.where(places < fixed, places, passed)]].set(jnp.asarray(tallies, jnp.int32))

    tallies = jnp.where(number % 4 == 0, named(packed, number // 4), named(common, number - number // 4 - 1))
    mixed = jax.random.permutation(jax.random.fold_in(own, 3), count)
    source_of, receiver = mixed[0:count // 2 * 2:2], mixed[1:count // 2 * 2:2]
    margin = jnp.minimum(tallies[source_of] - 1, reach - tallies[receiver]) // 2
    margin = jnp.where((source_of == sequence[0]) | (receiver == sequence[0]) | (tallies[receiver] == 0), 0, jnp.maximum(margin, 0))
    passed = jax.random.randint(jax.random.fold_in(own, 4), (count // 2,), 0, 1 << 20) % (margin + 1)
    tallies = tallies.at[source_of].add(-passed).at[receiver].add(passed)
    labels = jnp.searchsorted(jnp.cumsum(tallies), jnp.arange(rows * top), side="right").astype(jnp.int32)
    grid = labels.reshape(top, rows).T
    grid = grid[jax.random.permutation(jax.random.fold_in(own, 1), rows)]
    rotation = jax.random.randint(jax.random.fold_in(own, 2), (rows, 1), 0, top)
    return jnp.take_along_axis(grid, (jnp.arange(top)[None, :] + rotation) % top, axis=1)


def shares(count, total, limit, lean, full):
    loads = [(1 << 20) // math.isqrt(rank ** lean) + 1 for rank in range(1, count + 1)]
    largest = limit if full else min(limit, max(-(-total // count), total * loads[0] // sum(loads)))
    least = 1 if total - largest >= count - 1 else 0
    counts, surplus = [largest] + [least] * (count - 1), total - largest - least * (count - 1)
    while surplus > 0:
        candidates = [i for i in range(1, count) if counts[i] < largest] or [i for i in range(1, count) if counts[i] < limit]
        pool, remaining = sum([loads[i] for i in candidates]), surplus
        for i in candidates:
            addition = min(limit - counts[i], max(1, remaining * loads[i] // pool), surplus)
            counts[i] = counts[i] + addition
            surplus = surplus - addition
    return np.array(counts)


def scatter_about(own_key, extent, scale, most, cuts=(), held_as=jnp.bfloat16):
    drawn = jax.random.normal(own_key, extent, jnp.float32) * scale
    if len(cuts) > 0:
        drawn = shard_levels(own_key, extent, cuts, -0.22, 0.18) * drawn
    return jnp.clip(drawn, min=-most, max=most).astype(held_as)


def setup_inputs(seed: int = 0) -> dict:
    keys = jax.random.split(jax.random.key(seed), 20)
    query_a = scatter_about(keys[0], (TOKEN_TOTAL, HEAD_TOTAL * DK), 1.0, 6.0, ((0, 8), (1, 4)))
    key_a = scatter_about(keys[1], (TOKEN_TOTAL, HEAD_TOTAL * DK), 1.0, 6.0, ((0, 8), (1, 4)))
    value_a = scatter_about(keys[2], (TOKEN_TOTAL, HEAD_TOTAL * DVA), 1.0, 6.0, ((0, 8), (1, 4)))
    query_b = scatter_about(keys[3], (TOKEN_TOTAL, HEAD_TOTAL * DK), 1.0, 6.0, ((0, 8), (1, 4)))
    key_b = scatter_about(keys[4], (TOKEN_TOTAL, HEAD_TOTAL * DK), 1.0, 6.0, ((0, 8), (1, 4)))
    value_b = scatter_about(keys[5], (TOKEN_TOTAL, HEAD_TOTAL * DVB), 1.0, 6.0, ((0, 8), (1, 4)))
    in_gate = draw_in_gate(jax.random.fold_in(keys[19], 71), 0)
    forget_gate = draw_forget_gate(jax.random.fold_in(keys[19], 71), 0)
    head_gain_a = jnp.clip(1.0 + 0.18 * jax.random.normal(keys[8], (HEAD_TOTAL, DVA), jnp.float32), 0.1, 1.9)
    head_gain_b = jnp.clip(1.0 + 0.18 * jax.random.normal(keys[9], (HEAD_TOTAL, DVB), jnp.float32), 0.1, 1.9)
    out_weight_a = scatter_about(keys[10], (HEAD_TOTAL * DVA, D), (HEAD_TOTAL * (DVA + DVB)) ** -0.5, 0.078125, ((0, 4),))
    out_weight_b = scatter_about(keys[11], (HEAD_TOTAL * DVB, D), (HEAD_TOTAL * (DVA + DVB)) ** -0.5, 0.078125, ((0, 4),))
    residual = draw_residual(jax.random.fold_in(keys[19], 71), 0)
    norm_gain = jnp.clip(1.0 + 0.18 * jax.random.normal(keys[13], (D,), jnp.float32), 0.1, 1.9)
    routes_keys = jax.random.split(jax.random.fold_in(keys[14], 1), TOKEN_TOTAL // TOK_DEV)
    routes_turns = jax.random.permutation(jax.random.fold_in(keys[14], 3), TOKEN_TOTAL // TOK_DEV)
    routes = jax.vmap(lambda own, number: deal_out(jax.random.fold_in(keys[14], 2), own, number, TOK_DEV, EXPERTS, TOP, SLOTS, 3))(routes_keys, routes_turns).reshape((TOKEN_TOTAL, TOP))
    route_weights = jnp.clip(0.2 + 0.8 * jax.random.uniform(keys[15], (TOKEN_TOTAL, TOP), jnp.float32) ** shard_levels(keys[15], (TOKEN_TOTAL, TOP), ((0, 8),), -0.2, 0.2), 0.2, 1.0)
    expert_gate = scatter_about(keys[16], (EXPERTS, D, FF), D ** -0.5, 0.125, ((0, 8), (2, 4)))
    expert_up = scatter_about(keys[17], (EXPERTS, D, FF), D ** -0.5, 0.125, ((0, 8), (2, 4)))
    expert_down = scatter_about(keys[18], (EXPERTS, FF, D), FF ** -0.5, 0.09375, ((0, 8), (1, 4)))
    return dict(query_a=query_a, key_a=key_a, value_a=value_a, query_b=query_b, key_b=key_b, value_b=value_b, in_gate=in_gate, forget_gate=forget_gate, head_gain_a=head_gain_a, head_gain_b=head_gain_b, out_weight_a=out_weight_a, out_weight_b=out_weight_b, residual=residual, norm_gain=norm_gain, routes=routes, route_weights=route_weights, expert_gate=expert_gate, expert_up=expert_up, expert_down=expert_down)


EPSILON = 1e-06

def one_direction(queries, keys_in, values_in, log_input, log_decay):
    head_count, length, width_k = queries.shape
    blocks = length // BLOCK
    lower_mask = jnp.tril(jnp.ones((BLOCK, BLOCK), dtype=bool))

    def to_blocks(tensor):
        return jnp.moveaxis(tensor.reshape(head_count, blocks, BLOCK, *tensor.shape[2:]), 1, 0)

    def block_step(carried_state, inputs_block):
        memory, normal, stabilizer = carried_state
        q_block, k_block, v_block, in_block, decay_block = inputs_block
        cumulative = jnp.cumsum(decay_block, axis=-1)
        running_log_decay = cumulative + stabilizer[:, None]
        log_weights = jnp.where(lower_mask, cumulative[:, :, None] - cumulative[:, None, :] + in_block[:, None, :], -jnp.inf)
        row_peak = jnp.maximum(running_log_decay, lax.optimization_barrier(jnp.max(log_weights, axis=-1)))
        carried_weight = jnp.exp(running_log_decay - row_peak)
        scores = jnp.einsum('htd,hsd->hts', q_block, k_block) * jnp.exp(log_weights - row_peak[:, :, None])
        rounded = lax.optimization_barrier(scores.astype(jnp.bfloat16)).astype(jnp.float32)
        numerator = carried_weight[:, :, None] * jnp.einsum('htd,hde->hte', q_block, memory) + jnp.einsum('hts,hse->hte', rounded, v_block)
        denominator = carried_weight * jnp.einsum('htd,hd->ht', q_block, normal) + lax.optimization_barrier(jnp.sum(scores, axis=-1))
        outputs = numerator / jnp.maximum(jnp.abs(denominator), jnp.exp(-row_peak))[:, :, None]
        decay_total = cumulative[:, -1]
        tail_logs = decay_total[:, None] - cumulative + in_block
        new_stabilizer = jnp.maximum(decay_total + stabilizer, lax.optimization_barrier(jnp.max(tail_logs, axis=-1)))
        keep_scale = jnp.exp(decay_total + stabilizer - new_stabilizer)
        weighted_keys = k_block * jnp.exp(tail_logs - new_stabilizer[:, None])[:, :, None]
        memory = keep_scale[:, None, None] * memory + jnp.einsum('hsd,hse->hde', weighted_keys, v_block)
        normal = keep_scale[:, None] * normal + lax.optimization_barrier(jnp.sum(weighted_keys, axis=1))
        return ((memory, normal, new_stabilizer), outputs)
    start = (jnp.zeros((head_count, width_k, values_in.shape[-1]), jnp.float32), jnp.zeros((head_count, width_k), jnp.float32), jnp.zeros((head_count,), jnp.float32))
    blocked = tuple((to_blocks(tensor) for tensor in (queries, keys_in, values_in, log_input, log_decay)))
    final_state, outputs = lax.scan(block_step, start, blocked)
    return jnp.moveaxis(outputs, 0, 1).reshape(head_count, length, -1)

def mixer_group(queries, keys_in, values_in, log_input, log_decay, head_gain):
    width_k = queries.shape[1] // HEAD_TOTAL
    width_v = values_in.shape[1] // HEAD_TOTAL
    q_heads = queries.astype(jnp.float32).reshape(TOKEN_TOTAL, HEAD_TOTAL, width_k).transpose(1, 0, 2) * width_k ** (-0.5)
    k_heads = keys_in.astype(jnp.float32).reshape(TOKEN_TOTAL, HEAD_TOTAL, width_k).transpose(1, 0, 2)
    v_heads = values_in.astype(jnp.float32).reshape(TOKEN_TOTAL, HEAD_TOTAL, width_v).transpose(1, 0, 2)
    forward = one_direction(q_heads, k_heads, v_heads, log_input[0], log_decay[0])
    backward = jnp.flip(one_direction(jnp.flip(q_heads, 1), jnp.flip(k_heads, 1), jnp.flip(v_heads, 1), jnp.flip(log_input[1], 1), jnp.flip(log_decay[1], 1)), 1)
    both = forward + backward
    scaled = both * lax.rsqrt(lax.optimization_barrier(jnp.mean(both * both, axis=-1, keepdims=True)) + EPSILON) * head_gain[:, None, :]
    return scaled.astype(jnp.bfloat16).transpose(1, 0, 2).reshape(TOKEN_TOTAL, HEAD_TOTAL * width_v)

def reference(query_a, key_a, value_a, query_b, key_b, value_b, in_gate, forget_gate, head_gain_a, head_gain_b, out_weight_a, out_weight_b, residual, norm_gain, routes, route_weights, expert_gate, expert_up, expert_down):
    log_decay = jax.nn.log_sigmoid(forget_gate)
    heads_a = mixer_group(query_a, key_a, value_a, in_gate[:, 0], log_decay[:, 0], head_gain_a)
    heads_b = mixer_group(query_b, key_b, value_b, in_gate[:, 1], log_decay[:, 1], head_gain_b)
    mix = jnp.dot(heads_a, out_weight_a, preferred_element_type=jnp.float32) + jnp.dot(heads_b, out_weight_b, preferred_element_type=jnp.float32)
    updated = residual.astype(jnp.float32) + mix.T
    squares = lax.optimization_barrier(jnp.sum(updated * updated, axis=0))
    normed = (updated * lax.rsqrt(squares / D + EPSILON)[None, :] * norm_gain[:, None]).astype(jnp.bfloat16)
    token_rows = normed.T
    flat_routes = routes.reshape(N_SP, TOK_DEV * TOP)
    hits = (flat_routes[:, :, None] == jnp.arange(EXPERTS, dtype=jnp.int32)[None, None, :]).astype(jnp.int32)
    ranks = lax.optimization_barrier(jnp.sum((jnp.cumsum(hits, axis=1) - 1) * hits, axis=2))
    token_positions = (jnp.arange(N_SP, dtype=jnp.int32)[:, None] * SLOTS + ranks).reshape(TOKEN_TOTAL, TOP).astype(jnp.int32)
    owners = jnp.broadcast_to(jnp.arange(TOKEN_TOTAL, dtype=jnp.int32)[:, None], (TOKEN_TOTAL, TOP))
    table = jnp.zeros((EXPERTS, N_SP * SLOTS), jnp.int32).at[routes, token_positions].set(owners)
    group_width = FF // N_TP

    def one_expert(inputs_expert):
        gate_matrix, up_matrix, down_matrix, row_ids = inputs_expert
        rows = jnp.take(token_rows, row_ids, axis=0)
        gate = jnp.dot(rows, gate_matrix, preferred_element_type=jnp.float32)
        upward = jnp.dot(rows, up_matrix, preferred_element_type=jnp.float32)
        hidden = (jax.nn.silu(gate) * upward).astype(jnp.bfloat16)
        pieces = jnp.einsum('rjg,jgd->jrd', hidden.reshape(-1, N_TP, group_width).astype(jnp.float32), down_matrix.reshape(N_TP, group_width, D).astype(jnp.float32))
        pieces = lax.optimization_barrier(pieces.astype(jnp.bfloat16)).astype(jnp.float32)
        return lax.optimization_barrier(jnp.sum(pieces, axis=0)).astype(jnp.bfloat16)
    expert_rows = lax.map(one_expert, (expert_gate, expert_up, expert_down, table))
    picked = expert_rows[routes, token_positions].astype(jnp.float32)
    combined = updated + lax.optimization_barrier(jnp.sum(route_weights[:, :, None] * picked, axis=1)).T
    return combined.astype(jnp.bfloat16)
```

```python
import jax
import jax.numpy as jnp
from jax import lax
from jax.experimental import pallas as pl
from jax.experimental.pallas import tpu as pltpu
from jax.sharding import PartitionSpec as P

EPSILON = 1e-06
NOTHING = -1e30


def dot(left, right, contract):
    return lax.dot_general(
        left, right, (contract, ((), ())), preferred_element_type=jnp.float32
    )


def one_head(query, key, value, keys, values, inner_row, outer_row, column, peak, gain):
    length, width_k = query.shape
    scale = width_k ** (-0.5)
    rows = lax.broadcasted_iota(jnp.int32, (length, length), 0)
    lanes = lax.broadcasted_iota(jnp.int32, (length, length), 1)
    near = dot(query, key, ((1,), (1,))) * scale
    far = dot(query, keys, ((1,), (1,))) * scale
    far_scores = [far * outer_row[r] for r in range(2)]
    far_sums = [jnp.sum(scores, axis=1, keepdims=True) for scores in far_scores]
    far_values = dot(
        jnp.concatenate([scores.astype(jnp.bfloat16) for scores in far_scores], axis=0),
        values,
        ((1,), (0,)),
    )
    both = None
    for r in range(2):
        keep = lanes <= rows if r == 0 else lanes >= rows
        logs = jnp.where(keep, column[r] + inner_row[r], NOTHING)
        carried_log = column[r] + peak[r]
        top = jnp.maximum(carried_log, jnp.max(logs, axis=1, keepdims=True))
        carried = jnp.exp(carried_log - top)
        scores = near * jnp.exp(logs - top)
        numer = carried * far_values[r * length : (r + 1) * length] + dot(
            scores.astype(jnp.bfloat16), value, ((1,), (0,))
        )
        denom = carried * far_sums[r] + jnp.sum(scores, axis=1, keepdims=True)
        out = numer / jnp.maximum(jnp.abs(denom), jnp.exp(-top))
        both = out if both is None else both + out
    mean = jnp.mean(both * both, axis=1, keepdims=True)
    return (both * lax.rsqrt(mean + EPSILON) * gain).astype(jnp.bfloat16)


def mixer_kernel(
    qa, ka, va, qb, kb, vb, all_ka, all_va, all_kb, all_vb,
    inner, outer, column, peak, gain_a, gain_b, heads_a, heads_b,
):
    parts = (
        (qa, ka, va, all_ka, all_va, gain_a, heads_a),
        (qb, kb, vb, all_kb, all_vb, gain_b, heads_b),
    )
    for g, (q, k, v, every_k, every_v, gain, heads) in enumerate(parts):
        heads[...] = one_head(
            q[...], k[...], v[...], every_k[...], every_v[...],
            [inner[0, 2 * r + g : 2 * r + g + 1, :] for r in range(2)],
            [outer[0, 2 * r + g : 2 * r + g + 1, :] for r in range(2)],
            [column[0, :, 2 * r + g : 2 * r + g + 1] for r in range(2)],
            [peak[0, 2 * r + g : 2 * r + g + 1, 0:1] for r in range(2)],
            gain[0],
        )


def mix_heads(query_a, key_a, value_a, query_b, key_b, value_b, in_gate, forget_gate, gain_a, gain_b):
    heads = gain_a.shape[0]
    length = query_a.shape[0]
    width_k = query_a.shape[1] // heads
    width_a, width_b = gain_a.shape[1], gain_b.shape[1]
    count, mine = lax.axis_size("sp"), lax.axis_index("sp")
    packed = jnp.concatenate([value_a, key_a, key_b, value_b], axis=1)
    gathered = lax.all_gather(packed, "sp", axis=0, tiled=True)
    total_rows = gathered.shape[0]
    log_decay = jax.nn.log_sigmoid(forget_gate)
    ones = jnp.ones((length, length), jnp.float32)
    exact = lax.Precision.HIGHEST
    run = jnp.stack(
        [
            jnp.einsum("ghs,st->ght", log_decay[0], jnp.triu(ones), precision=exact),
            jnp.einsum("ghs,st->ght", log_decay[1], jnp.tril(ones), precision=exact),
        ]
    )
    whole = jnp.sum(log_decay, axis=-1, keepdims=True)
    tails = in_gate + whole - run
    small = lax.all_gather(
        jnp.stack([tails, jnp.broadcast_to(whole, tails.shape)]), "sp", axis=0
    )
    every_tail, every_whole = small[:, 0], small[:, 1, ..., 0]
    place = jnp.arange(count)
    source, middle = place[:, None], place[None, :]
    between = jnp.stack(
        [
            (middle > source) & (middle < mine),
            (middle < source) & (middle > mine),
        ]
    ).astype(jnp.float32)
    gap = jnp.sum(between[:, :, :, None, None] * jnp.moveaxis(every_whole, 0, 1)[:, None], axis=2)
    seen = jnp.stack([place < mine, place > mine])[:, :, None, None, None]
    logs = jnp.where(seen, jnp.moveaxis(every_tail, 0, 1) + gap[..., None], NOTHING)
    peak = jnp.max(logs, axis=(1, 4))
    outer = jnp.where(seen, jnp.exp(logs - peak[:, None, :, :, None]), 0.0)
    outer = outer.transpose(3, 0, 2, 1, 4).reshape(heads, 4, total_rows)
    peak = jnp.broadcast_to(peak.transpose(2, 0, 1).reshape(heads, 4, 1), (heads, 4, 128))
    inner = (in_gate - run).transpose(2, 0, 1, 3).reshape(heads, 4, length)
    column = run.transpose(2, 3, 0, 1).reshape(heads, length, 4)
    ratio = width_a // width_k

    def columns(rows, width, first):
        return pl.BlockSpec((rows, width), lambda h: (0, first + h))

    def by_head(*shape):
        return pl.BlockSpec((1,) + shape, lambda h: (h, 0, 0))

    return pl.pallas_call(
        mixer_kernel,
        grid=(heads,),
        in_specs=[
            columns(length, width_k, 0),
            columns(length, width_k, 0),
            columns(length, width_a, 0),
            columns(length, width_k, 0),
            columns(length, width_k, 0),
            columns(length, width_b, 0),
            columns(total_rows, width_k, ratio * heads),
            columns(total_rows, width_a, 0),
            columns(total_rows, width_k, (ratio + 1) * heads),
            columns(total_rows, width_b, (ratio + 2) * heads),
            by_head(4, length),
            by_head(4, total_rows),
            by_head(length, 4),
            by_head(4, 128),
            by_head(1, width_a),
            by_head(1, width_b),
        ],
        out_specs=[columns(length, width_a, 0), columns(length, width_b, 0)],
        out_shape=[
            jax.ShapeDtypeStruct((length, heads * width_a), jnp.bfloat16),
            jax.ShapeDtypeStruct((length, heads * width_b), jnp.bfloat16),
        ],
        cost_estimate=pl.CostEstimate(
            flops=4 * heads * length * total_rows * (2 * width_k + 2 * width_a),
            bytes_accessed=2 * packed.size * count,
            transcendentals=0,
        ),
    )(
        query_a, key_a, value_a, query_b, key_b, value_b,
        gathered, gathered, gathered, gathered,
        inner, outer, column, peak, gain_a[:, None, :], gain_b[:, None, :],
    )


def local(
    query_a,
    key_a,
    value_a,
    query_b,
    key_b,
    value_b,
    in_gate,
    forget_gate,
    head_gain_a,
    head_gain_b,
    out_weight_a,
    out_weight_b,
    residual,
    norm_gain,
    routes,
    route_weights,
    expert_gate,
    expert_up,
    expert_down,
):
    heads_a, heads_b = mix_heads(
        query_a, key_a, value_a, query_b, key_b, value_b,
        in_gate, forget_gate, head_gain_a, head_gain_b,
    )
    first_term = jnp.einsum("ec,se->cs", out_weight_a, heads_a, preferred_element_type=jnp.float32)
    mix = lax.psum_scatter(
        (
            first_term
            + jnp.einsum("ec,se->cs", out_weight_b, heads_b, preferred_element_type=jnp.float32)
        ).astype(jnp.bfloat16),
        "tp",
        scatter_dimension=0,
        tiled=True,
    ).astype(jnp.float32)
    updated = residual.astype(jnp.float32) + mix
    squares = lax.psum(jnp.sum(updated * updated, axis=0), "tp")
    whole_width = residual.shape[0] * lax.axis_size("tp")
    normed = (
        updated * lax.rsqrt(squares / whole_width + EPSILON)[None, :] * norm_gain[:, None]
    ).astype(jnp.bfloat16)
    token_count = routes.shape[0]
    top_count = routes.shape[1]
    expert_count = lax.axis_size("sp") * expert_gate.shape[0]
    slot_count = 2 * token_count * top_count // expert_count
    flat_routes = routes.reshape(-1)
    hits = (flat_routes[:, None] == jnp.arange(expert_count, dtype=jnp.int32)[None, :]).astype(
        jnp.int32
    )
    ranks = jnp.sum((jnp.cumsum(hits, axis=0) - 1) * hits, axis=1)
    targets = (flat_routes * slot_count + ranks).reshape(token_count, top_count)
    slot_ids = jnp.arange(expert_count * slot_count, dtype=jnp.int32)[:, None]
    selectors = [
        (slot_ids == targets[None, :, ordering_index]).astype(jnp.bfloat16)
        for ordering_index in range(top_count)
    ]
    dispatch = selectors[0]
    ordering_index = 1
    dispatch = dispatch + selectors[ordering_index]
    buffer = jnp.einsum("ps,ds->pd", dispatch, normed, preferred_element_type=jnp.float32)
    buffer = buffer.astype(jnp.bfloat16).reshape(expert_count, slot_count, -1)
    arrived = lax.all_to_all(buffer, "sp", split_axis=0, concat_axis=0, tiled=True)
    piece = lax.all_gather(arrived, "tp", axis=2, tiled=True)
    flat_rows = piece.reshape(-1, piece.shape[-1])
    gate_rows = expert_gate[0]
    up_rows = expert_up[0]
    gate = jnp.dot(flat_rows, gate_rows, preferred_element_type=jnp.float32)
    upward = jnp.dot(flat_rows, up_rows, preferred_element_type=jnp.float32)
    hidden = (
        (jax.nn.silu(gate) * upward)
        .astype(jnp.bfloat16)
        .reshape(arrived.shape[0], arrived.shape[1], -1)
    )
    sources = hidden.shape[0]
    hidden_rows = hidden.reshape(-1, hidden.shape[-1])
    columns = expert_down[0]
    summed = lax.psum_scatter(
        jnp.einsum("rf,fc->cr", hidden_rows, columns, preferred_element_type=jnp.float32).astype(
            jnp.bfloat16
        ),
        "tp",
        scatter_dimension=0,
        tiled=True,
    ).astype(jnp.float32)
    outgoing = summed.astype(jnp.bfloat16).reshape(summed.shape[0], sources, slot_count)
    returned = lax.all_to_all(outgoing, "sp", split_axis=1, concat_axis=1, tiled=True)
    returned = returned.reshape(returned.shape[0], -1)
    combined = updated
    for ordering_index in range(top_count):
        picked = jnp.dot(returned, selectors[ordering_index], preferred_element_type=jnp.float32)
        combined = combined + route_weights[:, ordering_index][None, :] * picked
    return combined.astype(jnp.bfloat16)


def solution(mesh):
    placed = (
        P("sp", "tp"),
        P("sp", "tp"),
        P("sp", "tp"),
        P("sp", "tp"),
        P("sp", "tp"),
        P("sp", "tp"),
        P(None, None, "tp", "sp"),
        P(None, None, "tp", "sp"),
        P("tp", None),
        P("tp", None),
        P("tp", None),
        P("tp", None),
        P("tp", "sp"),
        P("tp"),
        P("sp", None),
        P("sp", None),
        P("sp", None, "tp"),
        P("sp", None, "tp"),
        P("sp", "tp", None),
    )
    return jax.shard_map(
        local, mesh=mesh, in_specs=placed, out_specs=P("tp", "sp"), check_vma=False
    )
```

```python
import functools

import jax
import jax.numpy as jnp
from jax import lax
from jax.experimental import pallas as pl
from jax.experimental.pallas import tpu as pltpu
from jax.sharding import PartitionSpec as P

EPSILON = 1e-06
NOTHING = -1e30


def dot(left, right, contract):
    return lax.dot_general(
        left, right, (contract, ((), ())), preferred_element_type=jnp.float32
    )


MESH = pl.DeviceIdType.MESH


def greet(peers):
    barrier = pltpu.get_barrier_semaphore()
    for peer in peers:
        pl.semaphore_signal(barrier, inc=1, device_id=peer, device_id_type=MESH)
    pl.semaphore_wait(barrier, len(peers))


def exchange_kernel(count, arrays, *refs):
    given, taken = refs[:arrays], refs[arrays : 2 * arrays]
    sent, landed, kept = refs[2 * arrays :]
    mine = lax.axis_index("sp")
    peers = [lax.rem(mine + step, count) for step in range(1, count)]
    greet([{"sp": peer} for peer in peers])
    copies = []
    for step, peer in enumerate(peers):
        for a in range(arrays):
            copy = pltpu.make_async_remote_copy(
                src_ref=given[a].at[peer],
                dst_ref=taken[a].at[mine],
                send_sem=sent.at[a, step],
                recv_sem=landed.at[a, step],
                device_id={"sp": peer},
                device_id_type=MESH,
            )
            copy.start()
            copies.append(copy)
    for a in range(arrays):
        copy = pltpu.make_async_copy(given[a].at[mine], taken[a].at[mine], kept.at[a])
        copy.start()
        copies.append(copy)
    for copy in copies:
        copy.wait()


def exchange(arrays, number):
    count = arrays[0].shape[0]
    spec = pl.BlockSpec(memory_space=pltpu.VMEM)
    return pl.pallas_call(
        functools.partial(exchange_kernel, count, len(arrays)),
        out_shape=[jax.ShapeDtypeStruct(a.shape, a.dtype) for a in arrays],
        in_specs=[spec] * len(arrays),
        out_specs=[spec] * len(arrays),
        scratch_shapes=[
            pltpu.SemaphoreType.DMA((len(arrays), count - 1)),
            pltpu.SemaphoreType.DMA((len(arrays), count - 1)),
            pltpu.SemaphoreType.DMA((len(arrays),)),
        ],
        compiler_params=pltpu.CompilerParams(collective_id=number, has_side_effects=True),
    )(*arrays)


def dispatch_kernel(count, across, given, taken, sent, landed, kept, y_sent, y_landed, c_sent, c_landed):
    mine, slot = lax.axis_index("sp"), lax.axis_index("tp")
    chips = across // 2
    width = given.shape[-1]
    twin = slot + 1 - 2 * lax.rem(slot, 2)
    others = [lax.rem(slot + 2 * step, across) for step in range(1, chips)]
    behind = [lax.rem(slot + across - 2 * step, across) for step in range(1, chips)]
    peers = [lax.rem(mine + step, count) for step in range(1, count)]
    greet([{"sp": peer} for peer in peers] + [{"tp": other} for other in others] + [{"tp": twin}])

    def place(source, owner):
        return taken.at[source, :, pl.ds(pl.multiple_of(owner * width, width), width)]

    def forward(source, owner, target, send, land):
        copy = pltpu.make_async_remote_copy(
            src_ref=place(source, owner),
            dst_ref=place(source, owner),
            send_sem=send,
            recv_sem=land,
            device_id={"tp": target},
            device_id_type=MESH,
        )
        copy.start()
        return copy

    own = pltpu.make_async_copy(given.at[mine], place(mine, slot), kept.at[0])
    own.start()
    first = []
    for step, peer in enumerate(peers):
        copy = pltpu.make_async_remote_copy(
            src_ref=given.at[peer],
            dst_ref=place(mine, slot),
            send_sem=sent.at[step],
            recv_sem=landed.at[step],
            device_id={"sp": peer},
            device_id_type=MESH,
        )
        copy.start()
        first.append(copy)
    sources = [lax.rem(mine + count - step, count) for step in range(count)]
    along, last = [], []

    def hand_over(step):
        for turn, owner in enumerate(behind):
            along[step][turn].wait_recv()
            last.append(
                forward(
                    sources[step], owner, twin, c_sent.at[step, turn + 1], c_landed.at[step, turn + 1]
                )
            )

    for step in range(count):
        if step == 0:
            own.wait()
        else:
            first[step - 1].wait_recv()
        along.append(
            [
                forward(sources[step], slot, other, y_sent.at[step, turn], y_landed.at[step, turn])
                for turn, other in enumerate(others)
            ]
        )
        last.append(forward(sources[step], slot, twin, c_sent.at[step, 0], c_landed.at[step, 0]))
        if step > 0:
            hand_over(step - 1)
    hand_over(count - 1)
    for copy in first:
        copy.wait_send()
    for copies in along:
        for copy in copies:
            copy.wait_send()
    for copy in last:
        copy.wait()


def dispatch_rows(buffer, number):
    count, rows, width = buffer.shape
    across = lax.axis_size("tp")
    chips = across // 2
    spec = pl.BlockSpec(memory_space=pltpu.VMEM)
    dma = pltpu.SemaphoreType.DMA
    return pl.pallas_call(
        functools.partial(dispatch_kernel, count, across),
        out_shape=jax.ShapeDtypeStruct((count, rows, width * across), buffer.dtype),
        in_specs=[spec],
        out_specs=spec,
        scratch_shapes=[
            dma((count - 1,)), dma((count - 1,)), dma((1,)),
            dma((count, chips - 1)), dma((count, chips - 1)),
            dma((count, chips)), dma((count, chips)),
        ],
        compiler_params=pltpu.CompilerParams(collective_id=number, has_side_effects=True),
    )(buffer)


def one_head(query, key, value, keys, values, inner_row, outer_row, column, peak, gain, share):
    length, width_k = query.shape
    scale = width_k ** (-0.5)
    rows = lax.broadcasted_iota(jnp.int32, (length, length), 0)
    lanes = lax.broadcasted_iota(jnp.int32, (length, length), 1)
    near = dot(query, key, ((1,), (1,))) * scale
    far = dot(query, keys, ((1,), (1,))) * scale
    far_scores = [far * outer_row[r] for r in range(2)]
    far_sums = [jnp.sum(scores, axis=1, keepdims=True) for scores in far_scores]
    far_values = dot(
        jnp.concatenate([scores.astype(jnp.bfloat16) for scores in far_scores], axis=0),
        values,
        ((1,), (0,)),
    )
    both = None
    for r in range(2):
        keep = lanes <= rows if r == 0 else lanes >= rows
        logs = jnp.where(keep, column[r] + inner_row[r], NOTHING)
        carried_log = column[r] + peak[r]
        top = jnp.maximum(carried_log, jnp.max(logs, axis=1, keepdims=True))
        carried = jnp.exp(carried_log - top)
        scores = near * jnp.exp(logs - top)
        numer = carried * far_values[r * length : (r + 1) * length] + dot(
            scores.astype(jnp.bfloat16), value, ((1,), (0,))
        )
        denom = carried * far_sums[r] + jnp.sum(scores, axis=1, keepdims=True)
        out = numer / jnp.maximum(jnp.abs(denom), jnp.exp(-top))
        both = out if both is None else both + out
    mean = jnp.sum(both * both, axis=1, keepdims=True) * share
    return (both * lax.rsqrt(mean + EPSILON) * gain).astype(jnp.bfloat16)


def mixer_kernel(
    qa, ka, va, qb, kb, vb, all_ka, all_va, all_kb, all_vb,
    inner, outer, column, peak, gain_a, gain_b, heads_a, heads_b,
):
    parts = (
        (qa, ka, va, all_ka, all_va, gain_a, heads_a),
        (qb, kb, vb, all_kb, all_vb, gain_b, heads_b),
    )
    for g, (q, k, v, every_k, every_v, gain, heads) in enumerate(parts):
        heads[...] = one_head(
            q[...], k[...], v[...], every_k[...], every_v[...],
            [inner[0, 2 * r + g : 2 * r + g + 1, :] for r in range(2)],
            [outer[0, 2 * r + g : 2 * r + g + 1, :] for r in range(2)],
            [column[0, :, 2 * r + g : 2 * r + g + 1] for r in range(2)],
            [peak[0, 2 * r + g : 2 * r + g + 1, 0:1] for r in range(2)],
            gain[0],
            1.0 / gain.shape[-1],
        )


def mix_heads(query_a, key_a, value_a, query_b, key_b, value_b, in_gate, forget_gate, gain_a, gain_b):
    heads = gain_a.shape[0]
    length = query_a.shape[0]
    width_k = query_a.shape[1] // heads
    width_a, width_b = gain_a.shape[1], gain_b.shape[1]
    count, mine = lax.axis_size("sp"), lax.axis_index("sp")
    packed = jnp.concatenate([value_a, key_a, key_b, value_b], axis=1)
    gathered = lax.all_gather(packed, "sp", axis=0, tiled=True)
    total_rows = gathered.shape[0]
    log_decay = jax.nn.log_sigmoid(forget_gate)
    ones = jnp.ones((length, length), jnp.float32)
    exact = lax.Precision.HIGHEST
    run = jnp.stack(
        [
            jnp.einsum("ghs,st->ght", log_decay[0], jnp.triu(ones), precision=exact),
            jnp.einsum("ghs,st->ght", log_decay[1], jnp.tril(ones), precision=exact),
        ]
    )
    whole = jnp.sum(log_decay, axis=-1, keepdims=True)
    tails = in_gate + whole - run
    small = lax.all_gather(
        jnp.stack([tails, jnp.broadcast_to(whole, tails.shape)]), "sp", axis=0
    )
    every_tail, every_whole = small[:, 0], small[:, 1, ..., 0]
    place = jnp.arange(count)
    source, middle = place[:, None], place[None, :]
    between = jnp.stack(
        [
            (middle > source) & (middle < mine),
            (middle < source) & (middle > mine),
        ]
    ).astype(jnp.float32)
    gap = jnp.sum(between[:, :, :, None, None] * jnp.moveaxis(every_whole, 0, 1)[:, None], axis=2)
    seen = jnp.stack([place < mine, place > mine])[:, :, None, None, None]
    logs = jnp.where(seen, jnp.moveaxis(every_tail, 0, 1) + gap[..., None], NOTHING)
    peak = jnp.max(logs, axis=(1, 4))
    outer = jnp.where(seen, jnp.exp(logs - peak[:, None, :, :, None]), 0.0)
    outer = outer.transpose(3, 0, 2, 1, 4).reshape(heads, 4, total_rows)
    peak = jnp.broadcast_to(peak.transpose(2, 0, 1).reshape(heads, 4, 1), (heads, 4, 128))
    inner = (in_gate - run).transpose(2, 0, 1, 3).reshape(heads, 4, length)
    column = run.transpose(2, 3, 0, 1).reshape(heads, length, 4)
    ratio = width_a // width_k

    def columns(rows, width, first):
        return pl.BlockSpec((rows, width), lambda h: (0, first + h))

    def by_head(*shape):
        return pl.BlockSpec((1,) + shape, lambda h: (h, 0, 0))

    return pl.pallas_call(
        mixer_kernel,
        grid=(heads,),
        in_specs=[
            columns(length, width_k, 0),
            columns(length, width_k, 0),
            columns(length, width_a, 0),
            columns(length, width_k, 0),
            columns(length, width_k, 0),
            columns(length, width_b, 0),
            columns(total_rows, width_k, ratio * heads),
            columns(total_rows, width_a, 0),
            columns(total_rows, width_k, (ratio + 1) * heads),
            columns(total_rows, width_b, (ratio + 2) * heads),
            by_head(4, length),
            by_head(4, total_rows),
            by_head(length, 4),
            by_head(4, 128),
            by_head(1, width_a),
            by_head(1, width_b),
        ],
        out_specs=[columns(length, width_a, 0), columns(length, width_b, 0)],
        out_shape=[
            jax.ShapeDtypeStruct((length, heads * width_a), jnp.bfloat16),
            jax.ShapeDtypeStruct((length, heads * width_b), jnp.bfloat16),
        ],
        cost_estimate=pl.CostEstimate(
            flops=4 * heads * length * total_rows * (2 * width_k + 2 * width_a),
            bytes_accessed=2 * packed.size * count,
            transcendentals=0,
        ),
    )(
        query_a, key_a, value_a, query_b, key_b, value_b,
        gathered, gathered, gathered, gathered,
        inner, outer, column, peak, gain_a[:, None, :], gain_b[:, None, :],
    )


def unit_kernel(q, k, v, every_k, every_v, inner, outer, column, peak, gain, share, heads):
    heads[0] = one_head(
        q[0], k[0], v[0], every_k[...].reshape(-1, every_k.shape[-1]),
        every_v[...].reshape(-1, every_v.shape[-1]),
        [inner[0, r : r + 1, :] for r in range(2)],
        [outer[0, r : r + 1, :] for r in range(2)],
        [column[0, :, r : r + 1] for r in range(2)],
        [peak[0, r : r + 1, 0:1] for r in range(2)],
        gain[...],
        share[0:1, 0:1],
    )


def mix_units(query_a, key_a, value_a, query_b, key_b, value_b, in_gate, forget_gate, gain_a, gain_b):
    heads = gain_a.shape[0]
    length = query_a.shape[0]
    width_k = query_a.shape[1] // heads
    width_a, width_b = gain_a.shape[1], gain_b.shape[1]
    count, mine = lax.axis_size("sp"), lax.axis_index("sp")

    def widen(array, axis):
        pads = [(0, 0)] * array.ndim
        pads[axis] = (0, width_a - width_b)
        return jnp.pad(array, pads)

    def cut(values, queries, keys, width):
        parts = []
        for h in range(heads):
            value = values[:, h * width : (h + 1) * width]
            parts.append(
                jnp.concatenate(
                    [
                        value if width == width_a else widen(value, 1),
                        queries[:, h * width_k : (h + 1) * width_k],
                        keys[:, h * width_k : (h + 1) * width_k],
                    ],
                    axis=1,
                )
            )
        return parts

    packed = jnp.stack(
        cut(value_a, query_a, key_a, width_a) + cut(value_b, query_b, key_b, width_b)
    )
    log_decay = jax.nn.log_sigmoid(forget_gate)
    gates = jnp.stack([in_gate, log_decay], axis=2)
    gates = gates.transpose(1, 3, 0, 2, 4).reshape(count, 4, length)
    gates = jnp.concatenate([gates, jnp.zeros_like(gates)], axis=1)
    rows, gates = exchange([packed, gates], 0)
    in_rows, decay = gates[:, 0:4:2], gates[:, 1:4:2]
    ones = jnp.ones((length, length), jnp.float32)
    exact = lax.Precision.HIGHEST
    run = jnp.stack(
        [
            jnp.dot(decay[:, 0], jnp.triu(ones), precision=exact),
            jnp.dot(decay[:, 1], jnp.tril(ones), precision=exact),
        ],
        axis=1,
    )
    whole = jnp.sum(decay, axis=-1)
    tails = in_rows + whole[..., None] - run
    place = jnp.arange(count)
    reader, source, middle = place[:, None, None], place[None, :, None], place[None, None, :]
    between = jnp.stack(
        [
            (middle > source) & (middle < reader),
            (middle < source) & (middle > reader),
        ],
        axis=1,
    ).astype(jnp.float32)
    gap = jnp.sum(between * whole.T[None, :, None, :], axis=-1)
    seen = jnp.stack([source < reader, source > reader], axis=1)
    logs = jnp.where(seen, tails.transpose(1, 0, 2)[None] + gap[..., None], NOTHING)
    peak = jnp.max(logs, axis=(2, 3))
    outer = jnp.where(seen, jnp.exp(logs - peak[:, :, None, None]), 0.0)
    outer = outer.reshape(count, 2, count * length)
    peak = jnp.broadcast_to(peak[:, :, None], (count, 2, 128))
    inner = in_rows - run
    column = run.transpose(0, 2, 1)
    gains = jnp.concatenate([gain_a, widen(gain_b, 1)], axis=0)
    gain = lax.dynamic_slice_in_dim(gains, mine, 1, 0)
    share = jnp.full((1, 128), jnp.where(mine < heads, 1.0 / width_a, 1.0 / width_b), jnp.float32)
    first_q, first_k = width_a // width_k, width_a // width_k + 1

    def block(width, first):
        return pl.BlockSpec((1, length, width), lambda t: (t, 0, first))

    def every(width, first):
        return pl.BlockSpec((count, length, width), lambda t: (0, 0, first))

    def by_block(*shape):
        return pl.BlockSpec((1,) + shape, lambda t: (t, 0, 0))

    def fixed(*shape):
        return pl.BlockSpec(shape, lambda t: (0, 0))

    out = pl.pallas_call(
        unit_kernel,
        grid=(count,),
        in_specs=[
            block(width_k, first_q),
            block(width_k, first_k),
            block(width_a, 0),
            every(width_k, first_k),
            every(width_a, 0),
            by_block(2, length),
            by_block(2, count * length),
            by_block(length, 2),
            by_block(2, 128),
            fixed(1, width_a),
            fixed(1, 128),
        ],
        out_specs=block(width_a, 0),
        out_shape=jax.ShapeDtypeStruct((count, length, width_a), jnp.bfloat16),
    )(rows, rows, rows, rows, rows, inner, outer, column, peak, gain, share)
    (units,) = exchange([out], 1)

    def lay(parts):
        return jnp.concatenate(parts, axis=1)

    return (
        lay([units[h] for h in range(heads)]),
        lay([units[heads + h][:, :width_b] for h in range(heads)]),
    )


def local(
    query_a,
    key_a,
    value_a,
    query_b,
    key_b,
    value_b,
    in_gate,
    forget_gate,
    head_gain_a,
    head_gain_b,
    out_weight_a,
    out_weight_b,
    residual,
    norm_gain,
    routes,
    route_weights,
    expert_gate,
    expert_up,
    expert_down,
):
    whole_heads = 2 * head_gain_a.shape[0] == lax.axis_size("sp")
    heads_a, heads_b = (mix_units if whole_heads else mix_heads)(
        query_a, key_a, value_a, query_b, key_b, value_b,
        in_gate, forget_gate, head_gain_a, head_gain_b,
    )
    first_term = jnp.einsum("ec,se->cs", out_weight_a, heads_a, preferred_element_type=jnp.float32)
    mix = lax.psum_scatter(
        (
            first_term
            + jnp.einsum("ec,se->cs", out_weight_b, heads_b, preferred_element_type=jnp.float32)
        ).astype(jnp.bfloat16),
        "tp",
        scatter_dimension=0,
        tiled=True,
    ).astype(jnp.float32)
    updated = residual.astype(jnp.float32) + mix
    squares = lax.psum(jnp.sum(updated * updated, axis=0), "tp")
    whole_width = residual.shape[0] * lax.axis_size("tp")
    normed = (
        updated * lax.rsqrt(squares / whole_width + EPSILON)[None, :] * norm_gain[:, None]
    ).astype(jnp.bfloat16)
    token_count = routes.shape[0]
    top_count = routes.shape[1]
    expert_count = lax.axis_size("sp") * expert_gate.shape[0]
    slot_count = 2 * token_count * top_count // expert_count
    flat_routes = routes.reshape(-1)
    hits = (flat_routes[:, None] == jnp.arange(expert_count, dtype=jnp.int32)[None, :]).astype(
        jnp.int32
    )
    ranks = jnp.sum((jnp.cumsum(hits, axis=0) - 1) * hits, axis=1)
    targets = (flat_routes * slot_count + ranks).reshape(token_count, top_count)
    slot_ids = jnp.arange(expert_count * slot_count, dtype=jnp.int32)[:, None]
    selectors = [
        (slot_ids == targets[None, :, ordering_index]).astype(jnp.bfloat16)
        for ordering_index in range(top_count)
    ]
    dispatch = selectors[0]
    ordering_index = 1
    dispatch = dispatch + selectors[ordering_index]
    buffer = jnp.einsum("ps,ds->pd", dispatch, normed, preferred_element_type=jnp.float32)
    buffer = buffer.astype(jnp.bfloat16).reshape(expert_count, slot_count, -1)
    piece = dispatch_rows(buffer, 2)
    flat_rows = piece.reshape(-1, piece.shape[-1])
    gate_rows = expert_gate[0]
    up_rows = expert_up[0]
    gate = jnp.dot(flat_rows, gate_rows, preferred_element_type=jnp.float32)
    upward = jnp.dot(flat_rows, up_rows, preferred_element_type=jnp.float32)
    hidden = (
        (jax.nn.silu(gate) * upward)
        .astype(jnp.bfloat16)
        .reshape(expert_count, slot_count, -1)
    )
    sources = hidden.shape[0]
    hidden_rows = hidden.reshape(-1, hidden.shape[-1])
    columns = expert_down[0]
    summed = lax.psum_scatter(
        jnp.einsum("rf,fc->cr", hidden_rows, columns, preferred_element_type=jnp.float32).astype(
            jnp.bfloat16
        ),
        "tp",
        scatter_dimension=0,
        tiled=True,
    ).astype(jnp.float32)
    outgoing = summed.astype(jnp.bfloat16).reshape(summed.shape[0], sources, slot_count)
    returned = lax.all_to_all(outgoing, "sp", split_axis=1, concat_axis=1, tiled=True)
    returned = returned.reshape(returned.shape[0], -1)
    combined = updated
    for ordering_index in range(top_count):
        picked = jnp.dot(returned, selectors[ordering_index], preferred_element_type=jnp.float32)
        combined = combined + route_weights[:, ordering_index][None, :] * picked
    return combined.astype(jnp.bfloat16)


def solution(mesh):
    placed = (
        P("sp", "tp"),
        P("sp", "tp"),
        P("sp", "tp"),
        P("sp", "tp"),
        P("sp", "tp"),
        P("sp", "tp"),
        P(None, None, "tp", "sp"),
        P(None, None, "tp", "sp"),
        P("tp", None),
        P("tp", None),
        P("tp", None),
        P("tp", None),
        P("tp", "sp"),
        P("tp"),
        P("sp", None),
        P("sp", None),
        P("sp", None, "tp"),
        P("sp", None, "tp"),
        P("sp", "tp", None),
    )
    return jax.shard_map(
        local, mesh=mesh, in_specs=placed, out_specs=P("tp", "sp"), check_vma=False
    )
```
